32 devices in a mesh: sp: 8 (over z, x), tp: 4 (over y, core).
Axes of the slice: x: 2, y: 2, z: 4, core: 2. Of those that a mesh axis runs over, the one named last changes fastest.
Arguments:
- inputs: bfloat16 [4096, 4096], P('sp', 'tp'), may hold values from -6 to 6
- w_value: bfloat16 [4096, 4096], P(None, 'tp'), may hold values from -0.09375 to 0.09375
- w_gate: bfloat16 [4096, 4096], P(None, 'tp'), may hold values from -0.09375 to 0.09375
- taps: bfloat16 [31, 4096], P(None, 'tp'), may hold values from -1 to 1
- ln_gain: float32 [4096], P('tp'), may hold values from 0.1 to 1.9
- w_out: bfloat16 [4096, 4096], P(None, 'tp'), may hold values from -0.09375 to 0.09375
- grad_out: bfloat16 [4096, 4096], P('sp', 'tp'), may hold values from -6 to 6
Outputs:
- grad_input: bfloat16 [4096, 4096], P('sp', 'tp')
- grad_value_w: float32 [4096, 4096], P('sp', 'tp')
- grad_gate_w: float32 [4096, 4096], P('sp', 'tp')
- grad_out_w: float32 [4096, 4096], P('sp', 'tp')
- grad_taps: float32 [31, 4096], P(None, 'tp')
- grad_gain: float32 [4096], P('tp')
The draws below stay inside these ranges and needn't reach their ends.
All inputs are finite; a program needn't handle non-finite values.
Results may differ from the reference program's by a relative error of at most 0.017.
Values may be sent and summed in bfloat16 or wider, within the bound.
No kernel may reach another device: no remote copies, remote signals or barrier semaphores. Data moves between devices by JAX's collectives and lax.ppermute only.
A program may use at most 128 MiB of HBM per device.

```python
import jax
import jax.numpy as jnp
from jax import lax

D = 4096
CONV = 31
SEQ = 4096
N_TP = 4


def with_spikes(result, key, source, target, shards_of, factor):
    def block_of(position):
        return (jnp.arange(result.shape[position]) // (result.shape[position] // shards_of)).reshape((-1,) + (1,) * (result.ndim - 1 - position))

    first = jax.random.permutation(key, shards_of)[block_of(target)]
    second = (block_of(target) + shards_of // 2) % shards_of
    return jnp.where((block_of(source) == first) | (block_of(source) == second), factor * result, result)


def block_scale(key, dims, cuts, low, high):
    def one(axis_at, shards_of):
        draws = jax.random.uniform(jax.random.fold_in(jax.random.fold_in(key, 6), axis_at), (shards_of,), jnp.float32, low / len(cuts), high / len(cuts))
        return jnp.repeat(jnp.exp(draws), dims[axis_at] // shards_of).reshape((-1,) + (1,) * (len(dims) - axis_at - 1))

    gain = one(*cuts[0])
    for cut in cuts[1:]:
        gain = gain * one(*cut)
    return gain


def noise(rng, shape, spread, limit, split=(), held_as=jnp.bfloat16):
    array = spread * jax.random.normal(rng, shape, jnp.float32)
    if split:
        array = array * block_scale(rng, shape, split, -0.22, 0.18)
    return jnp.clip(array, -limit, limit).astype(held_as)


def heavy_noise(own_key, extent, spread, bound, split, heavy, kind=jnp.bfloat16):
    drawn = spread * jax.random.normal(own_key, extent, jnp.float32)
    if split:
        drawn = drawn * block_scale(own_key, extent, split, -0.22, 0.18)
    return jnp.clip(with_spikes(drawn, jax.random.fold_in(own_key, 3), *heavy), -bound, bound).astype(kind)


def setup_inputs(seed: int = 0) -> dict:
    arg_keys = jax.random.split(jax.random.key(seed), 8)
    return {
        "inputs": heavy_noise(arg_keys[0], (SEQ, D), 1.0, 6.0, ((0, 8), (1, 4)), (0, 1, 8, 2.0)),
        "w_value": noise(arg_keys[1], (D, D), D ** -0.5, 0.09375, ((1, 4),)),
        "w_gate": noise(arg_keys[2], (D, D), D ** -0.5, 0.09375, ((1, 4),)),
        "taps": noise(arg_keys[3], (CONV, D), CONV ** -0.5, 1.0, ((1, 4),)),
        "ln_gain": jnp.clip(1.0 + 0.18 * jax.random.normal(arg_keys[4], (D,), jnp.float32), 0.1, 1.9),
        "w_out": noise(arg_keys[5], (D, D), D ** -0.5, 0.09375, ((1, 4),)),
        "grad_out": heavy_noise(arg_keys[6], (SEQ, D), 1.0, 6.0, ((0, 8), (1, 4)), (0, 1, 8, 2.0)),
    }


def contract_tokens(left, right):
    return lax.dot_general(left, right, (((0,), (0,)), ((), ())), preferred_element_type=jnp.float32)

def contract_channels(left, right):
    return lax.dot_general(left, right, (((1,), (1,)), ((), ())), preferred_element_type=jnp.float32)

def reference(inputs, w_value, w_gate, taps, ln_gain, w_out, grad_out):
    seq_len = inputs.shape[0]
    full_width = inputs.shape[1]
    radius = taps.shape[0] // 2
    pre_value = jnp.dot(inputs, w_value, preferred_element_type=jnp.float32)
    pre_gate = jnp.dot(inputs, w_gate, preferred_element_type=jnp.float32)
    gate_sigmoid = jax.nn.sigmoid(pre_gate)
    hidden = (pre_value * gate_sigmoid).astype(jnp.bfloat16)
    padded = jnp.pad(hidden.astype(jnp.float32), ((radius, radius), (0, 0)))
    tap_values = taps.astype(jnp.float32)
    convolved = jnp.zeros((seq_len, full_width), jnp.float32)
    for offset in range(taps.shape[0]):
        convolved = convolved + tap_values[offset] * padded[offset:offset + seq_len]
    mean = lax.optimization_barrier(jnp.sum(convolved, axis=1, keepdims=True)) / full_width
    variance = lax.optimization_barrier(jnp.sum(convolved * convolved, axis=1, keepdims=True)) / full_width - mean * mean
    inverse = lax.rsqrt(variance + 1e-06)
    normed = (convolved - mean) * inverse
    scaled = normed * ln_gain
    activated = jax.nn.silu(scaled).astype(jnp.bfloat16)
    grad_act = jnp.dot(grad_out, w_out, preferred_element_type=jnp.float32)
    sig_scaled = jax.nn.sigmoid(scaled)
    grad_scaled = grad_act * sig_scaled * (1.0 + scaled * (1.0 - sig_scaled))
    grad_gain = lax.optimization_barrier(jnp.sum(grad_scaled * normed, axis=0))
    grad_normed = grad_scaled * ln_gain
    first_sum = lax.optimization_barrier(jnp.sum(grad_normed, axis=1, keepdims=True)) / full_width
    second_sum = lax.optimization_barrier(jnp.sum(grad_normed * normed, axis=1, keepdims=True)) / full_width
    grad_conv = inverse * (grad_normed - first_sum - normed * second_sum)
    tap_rows = []
    for offset in range(taps.shape[0]):
        tap_rows.append(lax.optimization_barrier(jnp.sum(padded[offset:offset + seq_len] * grad_conv, axis=0)))
    grad_taps = jnp.stack(tap_rows, axis=0)
    grad_padded = jnp.pad(grad_conv, ((radius, radius), (0, 0)))
    grad_hidden = jnp.zeros((seq_len, full_width), jnp.float32)
    for offset in range(taps.shape[0]):
        begin = 2 * radius - offset
        grad_hidden = grad_hidden + tap_values[offset] * grad_padded[begin:begin + seq_len]
    grad_value = (grad_hidden * gate_sigmoid).astype(jnp.bfloat16)
    grad_gate = (grad_hidden * pre_value * gate_sigmoid * (1.0 - gate_sigmoid)).astype(jnp.bfloat16)
    grad_value_w = contract_tokens(inputs, grad_value)
    grad_gate_w = contract_tokens(inputs, grad_gate)
    grad_out_w = contract_tokens(grad_out, activated)
    block = full_width // N_TP
    total = jnp.zeros((seq_len, full_width), jnp.float32)
    for index in range(N_TP):
        lower = index * block
        partial_value = contract_channels(grad_value[:, lower:lower + block], w_value[:, lower:lower + block])
        partial_value = partial_value + contract_channels(grad_gate[:, lower:lower + block], w_gate[:, lower:lower + block])
        rounded = lax.optimization_barrier(partial_value.astype(jnp.bfloat16))
        total = total + rounded.astype(jnp.float32)
    grad_input = total.astype(jnp.bfloat16)
    return (grad_input, grad_value_w, grad_gate_w, grad_out_w, grad_taps, grad_gain)
```

```python
import jax
import jax.numpy as jnp
from jax import lax
from jax.sharding import PartitionSpec as P


def minor_size(count):
    return max(size for size in range(1, count + 1) if size * size <= count and count % size == 0)


def snake_place(device, count):
    minor = minor_size(count)
    major = count // minor
    high, low = device // minor, device % minor
    return low * major + high + (low % 2) * (major - 1 - 2 * high)


def snake_device(place, count):
    minor = minor_size(count)
    major = count // minor
    low, high = place // major, place % major
    return (high + (low % 2) * (major - 1 - 2 * high)) * minor + low


def send(value, axis, step):
    return lax.ppermute(value, axis, [(i, i ^ step) for i in range(lax.axis_size(axis))])


def shifted(value, axis, steps):
    count = lax.axis_size(axis)
    leading, last = (max(0, -steps), min(count, count - steps))
    return lax.ppermute(value, axis, [(source, source + steps) for source in range(leading, last)])


def summed_by_exchange(value, axis):
    step = 1
    while step < lax.axis_size(axis):
        value = value + send(value, axis, step)
        step *= 2
    return value


def contract_tokens(left, right):
    return lax.dot_general(
        left, right, (((0,), (0,)), ((), ())), preferred_element_type=jnp.float32
    )


def contract_channels(left, right):
    return lax.dot_general(
        left, right, (((1,), (1,)), ((), ())), preferred_element_type=jnp.float32
    )


def after(value, *others):
    return lax.optimization_barrier((value, *others))[0]


def gathered_pieces(value, across):
    pieces = [value, send(value, "tp", 1)]
    for block in across:
        pieces += [block, send(block, "tp", 1)]
    return pieces


def projected(pieces, weight, total=None):
    me = lax.axis_index("tp")
    for step, piece in pieces:
        width = piece.shape[1]
        rows = lax.dynamic_slice_in_dim(weight, (me ^ step) * width, width, axis=0)
        term = jnp.dot(piece, rows, preferred_element_type=jnp.float32)
        total = term if total is None else total + term
    return total


def convolved_inside(cells, taps):
    radius, rows = taps.shape[0] // 2, cells.shape[0]
    padded = jnp.pad(cells.astype(jnp.float32), ((radius, radius), (0, 0)))
    total = jnp.zeros(cells.shape, jnp.float32)
    for offset in range(taps.shape[0]):
        total = total + taps[offset] * padded[offset : offset + rows]
    return total


def convolved_edges(before, behind, taps):
    radius = taps.shape[0] // 2
    first = jnp.pad(before.astype(jnp.float32), ((0, radius), (0, 0)))
    last = jnp.pad(behind.astype(jnp.float32), ((radius, 0), (0, 0)))
    low = sum(taps[k] * first[k : k + radius] for k in range(radius))
    high = sum(taps[k] * last[k - radius : k] for k in range(radius + 1, taps.shape[0]))
    return low, high


def convolved_tokens(cells, taps):
    radius, rows = taps.shape[0] // 2, cells.shape[0]
    before = shifted(cells[rows - radius :], "sp", 1)
    behind = shifted(cells[:radius], "sp", -1)
    inside = lax.optimization_barrier(convolved_inside(cells, taps))
    low, high = convolved_edges(before, behind, taps)
    edges = jnp.concatenate(
        [low, jnp.zeros((rows - 2 * radius, cells.shape[1]), jnp.float32), high], axis=0
    )
    return inside + edges, before, behind


def ring_sums(streams, fillers):
    count = lax.axis_size("sp")
    order = [snake_device(at, count) for at in range(count)]
    here = snake_place(lax.axis_index("sp"), count)
    ahead = [(order[i], order[(i + 1) % count]) for i in range(count)]
    behind = [(target, source) for source, target in ahead]

    def part_of(columns, step, way):
        own_rows = columns.shape[1] // lax.axis_size("tp")
        block = columns.shape[1] // count
        first = snake_device((here + 2 * count - way * (1 + step)) % count, count) * block
        slot = (first // own_rows) ^ lax.axis_index("tp")
        return lax.dynamic_slice_in_dim(columns, slot * own_rows + first % own_rows, block, axis=1)

    held, given, last = [None] * len(streams), [], None
    for step in range(count - 1):
        for which, (columns, array, way) in enumerate(streams):
            if last is not None:
                array = after(array, last)
            total = contract_tokens(part_of(columns, step, way), array)
            if step:
                total = total + held[which].astype(jnp.float32)
            last = total.astype(jnp.bfloat16)
            held[which] = lax.ppermute(last, "sp", ahead if way == 1 else behind)
        for at, work in fillers:
            if at == step:
                last = work(last)
                given.append(last)
    own = [
        contract_tokens(part_of(columns, count - 1, way), after(array, last))
        for columns, array, way in streams
    ]
    own = lax.optimization_barrier(own)
    return [
        part + arrived.astype(jnp.float32) for part, arrived in zip(own, held)
    ], given


def local(inputs, w_value, w_gate, taps, ln_gain, w_out, grad_out):
    tok_rows = inputs.shape[0]
    own_width = w_value.shape[1]
    full_width = inputs.shape[1] * lax.axis_size("tp")
    taps_count = taps.shape[0]
    radius = taps_count // 2
    half = own_width // 2
    steps = range(2, lax.axis_size("tp"), 2)
    pieces = gathered_pieces(inputs, [send(inputs, "tp", step) for step in steps])
    held_grads = after(grad_out, pieces[1])
    grad_pieces = gathered_pieces(grad_out, [send(held_grads, "tp", step) for step in steps])
    pieces = list(enumerate(pieces))
    grad_pieces = list(enumerate(grad_pieces))
    pre_value = projected(pieces[:2], w_value)
    pre_gate = projected(pieces[:2], w_gate)
    grad_act = projected(grad_pieces[:2], w_out)
    far_pieces = [(step, after(piece, grad_act)) for step, piece in pieces[2:]]
    pre_value = projected(far_pieces, w_value, pre_value)
    pre_gate = projected(far_pieces, w_gate, pre_gate)
    gate_sigmoid = jax.nn.sigmoid(pre_gate)
    hidden = (pre_value * gate_sigmoid).astype(jnp.bfloat16)
    tap_values = taps.astype(jnp.float32)
    convolved, before, behind = convolved_tokens(hidden, tap_values)
    far_grads = [(step, after(piece, convolved)) for step, piece in grad_pieces[2:]]
    grad_act = projected(far_grads, w_out, grad_act)
    full_grads = jnp.concatenate([after(piece, convolved) for _, piece in grad_pieces], axis=1)
    sums = jnp.stack([jnp.sum(convolved, axis=1), jnp.sum(convolved * convolved, axis=1)], axis=0)
    sums = summed_by_exchange(sums, "tp")
    mean = (sums[0] / full_width)[:, None]
    variance = (sums[1] / full_width)[:, None] - mean * mean
    inverse = lax.rsqrt(variance + 1e-06)
    normed = (convolved - mean) * inverse
    scaled = normed * ln_gain
    activated = jax.nn.silu(scaled).astype(jnp.bfloat16)
    sig_scaled = jax.nn.sigmoid(scaled)
    grad_scaled = grad_act * sig_scaled * (1.0 + scaled * (1.0 - sig_scaled))
    gain_part = jnp.sum(grad_scaled * normed, axis=0)
    grad_normed = grad_scaled * ln_gain
    grad_sums = jnp.stack(
        [jnp.sum(grad_normed, axis=1), jnp.sum(grad_normed * normed, axis=1)], axis=0
    )
    grad_sums = summed_by_exchange(grad_sums, "tp")
    grad_conv = inverse * (
        grad_normed
        - (grad_sums[0] / full_width)[:, None]
        - normed * (grad_sums[1] / full_width)[:, None]
    )
    grad_conv = lax.optimization_barrier(grad_conv)
    grad_hidden, _, _ = convolved_tokens(grad_conv, tap_values[::-1])
    grad_value = (grad_hidden * gate_sigmoid).astype(jnp.bfloat16)
    grad_gate = (grad_hidden * pre_value * gate_sigmoid * (1.0 - gate_sigmoid)).astype(jnp.bfloat16)
    full_inputs = jnp.concatenate([after(piece, activated) for _, piece in pieces], axis=1)
    me = lax.axis_index("tp")
    model_width = inputs.shape[1]

    def input_block(step):
        def work(last):
            first = (me ^ step) * model_width
            values, gates = lax.optimization_barrier((grad_value, grad_gate, last))[:2]
            rows = lax.dynamic_slice_in_dim(w_value, first, model_width, axis=0)
            block = contract_channels(values, rows)
            rows = lax.dynamic_slice_in_dim(w_gate, first, model_width, axis=0)
            return (block + contract_channels(gates, rows)).astype(jnp.bfloat16)

        return work

    def tap_sums(last):
        padded = jnp.concatenate([before, hidden, behind], axis=0)
        padded = after(padded, last).astype(jnp.float32)
        rows = [
            jnp.sum(padded[offset : offset + tok_rows] * grad_conv, axis=0)
            for offset in range(taps_count)
        ]
        return jnp.stack(rows + [gain_part], axis=0)

    tp_count = lax.axis_size("tp")
    fillers = [(1 + at // 2, input_block(tp_count - 1 - at)) for at in range(tp_count)]
    fillers.append((1 + tp_count // 2, tap_sums))
    (out_low, out_high, value_low, gate_low, value_high, gate_high), given = ring_sums(
        (
            (full_grads, activated[:, :half], 1),
            (full_grads, activated[:, half:], -1),
            (full_inputs, grad_value[:, :half], 1),
            (full_inputs, grad_gate[:, :half], -1),
            (full_inputs, grad_value[:, half:], 1),
            (full_inputs, grad_gate[:, half:], -1),
        ),
        fillers,
    )
    grad_out_w = jnp.concatenate([out_low, out_high], axis=1)
    grad_value_w = jnp.concatenate([value_low, value_high], axis=1)
    grad_gate_w = jnp.concatenate([gate_low, gate_high], axis=1)
    grad_input = given[tp_count - 1].astype(jnp.float32)
    for step in range(1, tp_count):
        grad_input = grad_input + send(given[tp_count - 1 - step], "tp", step).astype(jnp.float32)
    grad_input = grad_input.astype(jnp.bfloat16)
    small = summed_by_exchange(given[tp_count], "sp")
    grad_taps, grad_gain = small[:-1], small[-1]
    return (grad_input, grad_value_w, grad_gate_w, grad_out_w, grad_taps, grad_gain)


def solution(mesh):
    in_specs = (
        P("sp", "tp"),
        P(None, "tp"),
        P(None, "tp"),
        P(None, "tp"),
        P("tp"),
        P(None, "tp"),
        P("sp", "tp"),
    )
    out_specs = (P("sp", "tp"), P("sp", "tp"), P("sp", "tp"), P("sp", "tp"), P(None, "tp"), P("tp"))
    return jax.shard_map(local, mesh=mesh, in_specs=in_specs, out_specs=out_specs, check_vma=False)
```
